32 devices in a mesh: sp: 16 (over z, y, x), tp: 2 (over core).
Axes of the slice: x: 2, y: 2, z: 4, core: 2. Of those that a mesh axis runs over, the one named last changes fastest.
Arguments:
- queries: bfloat16 [4096, 1024], P('sp', 'tp'), may hold values from -6 to 6
- key_vectors: bfloat16 [4096, 1024], P('sp', 'tp'), may hold values from -6 to 6
- value_vectors: bfloat16 [4096, 1024], P('sp', 'tp'), may hold values from -6 to 6
- gate_inputs: bfloat16 [4096, 1024], P('sp', 'tp'), may hold values from -6 to 6
- log_decay: float32 [4096, 16], P('sp', 'tp'), may hold values from -1 to 0
- head_gain: float32 [1024], P('tp'), may hold values from 0.1 to 1.9
- out_weight: bfloat16 [1024, 2048], P('tp'), may hold values from -0.1875 to 0.1875
- residual: bfloat16 [4096, 2048], P(('sp', 'tp')), may hold values from -6 to 6
- norm_gain: float32 [2048], replicated, may hold values from 0.1 to 1.9
- expert_ids: int32 [4096, 2], P(('sp', 'tp')), may hold values from 0 to 15, all different within a row; in each aligned block of 128 rows (0 to 127, 128 to 255, ...) at most 32 rows name the same one
- expert_weights: float32 [4096, 2], P(('sp', 'tp')), may hold values from 0.2 to 1
- gate_experts: bfloat16 [16, 2048, 3584], P('sp', None, 'tp'), may hold values from -0.125 to 0.125
- up_experts: bfloat16 [16, 2048, 3584], P('sp', None, 'tp'), may hold values from -0.125 to 0.125
- down_experts: bfloat16 [16, 3584, 2048], P('sp', 'tp'), may hold values from -0.09375 to 0.09375
Outputs:
- layer_out: bfloat16 [4096, 2048], P(('sp', 'tp'))
The draws below stay inside these ranges and needn't reach their ends.
Inputs may be any that keep to these rules, and one draw needn't show every extreme that they name: `expert_ids`: the 2 experts of a token differ. No expert is named more than 32 times in the rows of one device, and in some device some expert is named exactly 32 times.
All inputs are finite; a program needn't handle non-finite values.
Results may differ from the reference program's by a relative error of at most 0.014.
Values may be sent and summed in bfloat16 or wider, within the bound.
A program may use at most 128 MiB of HBM per device.

```python
import math
import jax
import jax.numpy as jnp
import numpy as np
from jax import lax

D = 2048
MEMORY_CHANNELS = 16
HD = 64
FF = 3584
TOP = 2
BLOCK = 128
TOK_DEV = 256
STRING_LENGTH = 4096
EXPERTS = 16
CAP = 32
N_SP = 16
N_TP = 2


def draw_log_decay(key, part):
    concurrent_lanes = jax.random.split(key, 7)
    fast_share = 0.5
    fast = jax.random.uniform(concurrent_lanes[0], (MEMORY_CHANNELS,), jnp.float32) < fast_share
    fast_rate = jax.random.uniform(concurrent_lanes[1], (MEMORY_CHANNELS,), jnp.float32, 1.0 / 100.0, 1.0 / 30.0)
    slow_rate = jax.random.uniform(concurrent_lanes[2], (MEMORY_CHANNELS,), jnp.float32, 0.2, 0.6) / STRING_LENGTH
    reference_shrink_speed = jnp.where(fast, fast_rate, slow_rate)
    shrink_multipliers = jnp.exp(jax.random.uniform(concurrent_lanes[3], (STRING_LENGTH // BLOCK, MEMORY_CHANNELS), jnp.float32, -0.7, 0.7))
    shrink_multipliers = jnp.repeat(shrink_multipliers, BLOCK, axis=0)
    stochastic_jitter = jax.random.uniform(concurrent_lanes[4], (STRING_LENGTH, MEMORY_CHANNELS), jnp.float32, 0.5, 1.5)
    spike_occurrences = jax.random.uniform(concurrent_lanes[5], (STRING_LENGTH, MEMORY_CHANNELS), jnp.float32) < 2.0 / STRING_LENGTH
    surviving_proportion = jax.random.uniform(concurrent_lanes[6], (STRING_LENGTH, MEMORY_CHANNELS), jnp.float32, 0.5, 0.8)
    closing_result = -reference_shrink_speed[None, :] * shrink_multipliers * stochastic_jitter + jnp.where(spike_occurrences, jnp.log(surviving_proportion), 0.0)
    return closing_result.astype(jnp.float32)


def steps_of(stream_key, dims, shards, smallest, largest):
    loudness = 1.0
    for position, shards_of in shards:
        draws = jax.random.uniform(jax.random.fold_in(jax.random.fold_in(stream_key, 6), position), (shards_of,), jnp.float32, smallest / len(shards), largest / len(shards))
        loudness = loudness * jnp.repeat(jnp.exp(draws), dims[position] // shards_of).reshape((-1,) + (1,) * (len(dims) - 1 - position))
    return loudness


def assign_block(rng, own, number, rows, count, top, most, lean):
    ranking = jax.random.permutation(rng, count)
    packed, usual = portions_of(count, rows * top, most, lean, True), portions_of(count, rows * top, most, lean, False)
    places = jnp.arange(count)

    def named(sizes, rotation):
        used = int((sizes > 0).sum())
        fixed = max(1, used // 4)
        moved = fixed + (places - fixed + rotation * (used - fixed)) % max(1, count - fixed)
        return jnp.zeros((count,), jnp.int32).at[ranking[jnp.where(places < fixed, places, moved)]].set(jnp.asarray(sizes, jnp.int32))

    sizes = jnp.where(number % 4 == 0, named(packed, number // 4), named(usual, number - number // 4 - 1))
    mixed = jax.random.permutation(jax.random.fold_in(own, 3), count)
    donor, receiver = mixed[0:count // 2 * 2:2], mixed[1:count // 2 * 2:2]
    slack = jnp.minimum(sizes[donor] - 1, most - sizes[receiver]) // 2
    slack = jnp.where((donor == ranking[0]) | (receiver == ranking[0]) | (sizes[receiver] == 0), 0, jnp.maximum(slack, 0))
    moved = jax.random.randint(jax.random.fold_in(own, 4), (count // 2,), 0, 1 << 20) % (slack + 1)
    sizes = sizes.at[donor].add(-moved).at[receiver].add(moved)
    items = jnp.searchsorted(jnp.cumsum(sizes), jnp.arange(rows * top), side="right").astype(jnp.int32)
    listing = items.reshape(top, rows).T
    listing = listing[jax.random.permutation(jax.random.fold_in(own, 1), rows)]
    rotation = jax.random.randint(jax.random.fold_in(own, 2), (rows, 1), 0, top)
    return jnp.take_along_axis(listing, (jnp.arange(top)[None, :] + rotation) % top, axis=1)


def portions_of(amount, total, limit, skew, full):
    weights = [(1 << 20) // math.isqrt(grade ** skew) + 1 for grade in range(1, amount + 1)]
    largest = limit if full else min(limit, max(-(-total // amount), total * weights[0] // sum(weights)))
    least = 1 if total - largest >= amount - 1 else 0
    counts, spare = [largest] + [least] * (amount - 1), total - largest - least * (amount - 1)
    while spare > 0:
        free = [i for i in range(1, amount) if counts[i] < largest] or [i for i in range(1, amount) if counts[i] < limit]
        pool, budget = sum([weights[i] for i in free]), spare
        for i in free:
            more = min(limit - counts[i], max(1, budget * weights[i] // pool), spare)
            counts[i] = counts[i] + more
            spare = spare - more
    return np.array(counts)


def normal_values(own_key, extent, width, reach, cuts=(), kind=jnp.bfloat16):
    values = width * jax.random.normal(own_key, extent, jnp.float32)
    if cuts:
        values = values * steps_of(own_key, extent, cuts, -0.22, 0.18)
    return jnp.clip(values, -reach, reach).astype(kind)


def setup_inputs(seed: int = 0) -> dict:
    streams_of = jax.random.split(jax.random.key(seed), 15)
    queries = normal_values(streams_of[0], (STRING_LENGTH, MEMORY_CHANNELS * HD), 1.0, 6.0, ((0, 16), (1, 2)))
    key_vectors = normal_values(streams_of[1], (STRING_LENGTH, MEMORY_CHANNELS * HD), 1.0, 6.0, ((0, 16), (1, 2)))
    value_vectors = normal_values(streams_of[2], (STRING_LENGTH, MEMORY_CHANNELS * HD), 1.0, 6.0, ((0, 16), (1, 2)))
    gate_inputs = normal_values(streams_of[3], (STRING_LENGTH, MEMORY_CHANNELS * HD), 1.0, 6.0, ((0, 16), (1, 2)))
    log_decay = draw_log_decay(jax.random.fold_in(streams_of[14], 71), 0)
    head_gain = jnp.clip(1.0 + 0.18 * jax.random.normal(streams_of[5], (MEMORY_CHANNELS * HD,), jnp.float32), 0.1, 1.9)
    out_weight = normal_values(streams_of[6], (MEMORY_CHANNELS * HD, D), (MEMORY_CHANNELS * HD) ** -0.5, 0.1875, ((0, 2),))
    residual = normal_values(streams_of[7], (STRING_LENGTH, D), 1.0, 6.0, ((0, 32),))
    norm_gain = jnp.clip(1.0 + 0.18 * jax.random.normal(streams_of[8], (D,), jnp.float32), 0.1, 1.9)
    expert_ids_keys = jax.random.split(jax.random.fold_in(streams_of[9], 1), STRING_LENGTH // (TOK_DEV // N_TP))
    expert_ids_turns = jax.random.permutation(jax.random.fold_in(streams_of[9], 3), STRING_LENGTH // (TOK_DEV // N_TP))
    expert_ids = jax.vmap(lambda own, number: assign_block(jax.random.fold_in(streams_of[9], 2), own, number, TOK_DEV // N_TP, EXPERTS, TOP, CAP, 1))(expert_ids_keys, expert_ids_turns).reshape((STRING_LENGTH, TOP))
    expert_weights = jnp.clip(0.2 + 0.8 * jax.random.uniform(streams_of[10], (STRING_LENGTH, TOP), jnp.float32) ** steps_of(streams_of[10], (STRING_LENGTH, TOP), ((0, 32),), -0.2, 0.2), 0.2, 1.0)
    gate_experts = normal_values(streams_of[11], (EXPERTS, D, FF), D ** -0.5, 0.125, ((0, 16), (2, 2)))
    up_experts = normal_values(streams_of[12], (EXPERTS, D, FF), D ** -0.5, 0.125, ((0, 16), (2, 2)))
    down_experts = normal_values(streams_of[13], (EXPERTS, FF, D), FF ** -0.5, 0.09375, ((0, 16), (1, 2)))
    return dict(queries=queries, key_vectors=key_vectors, value_vectors=value_vectors, gate_inputs=gate_inputs, log_decay=log_decay, head_gain=head_gain, out_weight=out_weight, residual=residual, norm_gain=norm_gain, expert_ids=expert_ids, expert_weights=expert_weights, gate_experts=gate_experts, up_experts=up_experts, down_experts=down_experts)


def rotate(block, places):
    half_size = block.shape[-1] // 2
    frequency = 10000.0 ** (-jnp.arange(half_size, dtype=jnp.float32) / half_size)
    angles = places.astype(jnp.float32)[:, None, None] * frequency
    first_half = block[..., :half_size]
    second = block[..., half_size:]
    return jnp.concatenate([first_half * jnp.cos(angles) - second * jnp.sin(angles), second * jnp.cos(angles) + first_half * jnp.sin(angles)], axis=-1)

def to_blocks(source, blocks):
    shaped = source.reshape((blocks, source.shape[0] // blocks) + source.shape[1:])
    return jnp.swapaxes(shaped, 1, 2)

def from_blocks(source):
    shaped = jnp.swapaxes(source, 1, 2)
    return shaped.reshape((shaped.shape[0] * shaped.shape[1],) + shaped.shape[2:])

def block_step(carried_state, inputs):
    query_rows, key_rows, value_rows, decay_rows = inputs
    cumulative = jnp.cumsum(decay_rows, axis=1)
    log_gaps = cumulative[:, :, None] - cumulative[:, None, :]
    offsets = jnp.arange(decay_rows.shape[1])
    causal = offsets[:, None] >= offsets[None, :]
    decay_weight = jnp.where(causal, jnp.exp(jnp.where(causal, log_gaps, 0.0)), 0.0)
    scores = jnp.einsum('htd,hsd->hts', query_rows, key_rows, precision=lax.Precision.HIGHEST) * decay_weight
    within = jnp.einsum('hts,hse->hte', scores, value_rows, precision=lax.Precision.HIGHEST)
    carried = jnp.einsum('htd,hde->hte', query_rows * jnp.exp(cumulative)[:, :, None], carried_state, precision=lax.Precision.HIGHEST)
    last_log = cumulative[:, -1:]
    fresh_state = jnp.einsum('hsd,hse->hde', key_rows * jnp.exp(last_log - cumulative)[:, :, None], value_rows, precision=lax.Precision.HIGHEST)
    return (jnp.exp(last_log)[:, :, None] * carried_state + fresh_state, within + carried)

def round_trip(array):
    return lax.optimization_barrier(array.astype(jnp.bfloat16)).astype(jnp.float32)

def reference(queries, key_vectors, value_vectors, gate_inputs, log_decay, head_gain, out_weight, residual, norm_gain, expert_ids, expert_weights, gate_experts, up_experts, down_experts):
    places = jnp.arange(STRING_LENGTH, dtype=jnp.int32)
    turned_queries = rotate(queries.astype(jnp.float32).reshape(STRING_LENGTH, MEMORY_CHANNELS, HD), places)
    turned_keys = rotate(key_vectors.astype(jnp.float32).reshape(STRING_LENGTH, MEMORY_CHANNELS, HD), places) * HD ** (-0.5)
    value_float = value_vectors.astype(jnp.float32).reshape(STRING_LENGTH, MEMORY_CHANNELS, HD)
    blocks = STRING_LENGTH // BLOCK
    inputs = (to_blocks(turned_queries, blocks), to_blocks(turned_keys, blocks), to_blocks(value_float, blocks), to_blocks(log_decay, blocks))
    _, pieces = lax.scan(block_step, jnp.zeros((MEMORY_CHANNELS, HD, HD), jnp.float32), inputs)
    retained = from_blocks(pieces)
    squares = lax.optimization_barrier(jnp.mean(retained * retained, axis=-1, keepdims=True))
    normed = retained * lax.rsqrt(squares + 1e-06) * head_gain.reshape(MEMORY_CHANNELS, HD)
    normed = (normed.reshape(STRING_LENGTH, MEMORY_CHANNELS * HD) * jax.nn.silu(gate_inputs.astype(jnp.float32))).astype(jnp.bfloat16)
    half_heads = MEMORY_CHANNELS * HD // N_TP
    projected = jnp.zeros((STRING_LENGTH, D), jnp.float32)
    for section in range(N_TP):
        partial_value = jnp.dot(normed[:, section * half_heads:(section + 1) * half_heads], out_weight[section * half_heads:(section + 1) * half_heads], preferred_element_type=jnp.float32)
        projected = projected + round_trip(partial_value)
    mixed_rows = (residual.astype(jnp.float32) + projected).astype(jnp.bfloat16)
    mixed_float = mixed_rows.astype(jnp.float32)
    normed_rows = (mixed_float * lax.rsqrt(lax.optimization_barrier(jnp.mean(mixed_float * mixed_float, axis=-1, keepdims=True)) + 1e-06) * norm_gain).astype(jnp.bfloat16)
    sources = N_SP * N_TP
    flat_routes = expert_ids.reshape(sources, -1)
    onehot = (flat_routes[:, :, None] == jnp.arange(EXPERTS, dtype=jnp.int32)[None, None, :]).astype(jnp.int32)
    slot_rank = lax.optimization_barrier(jnp.sum(jnp.cumsum(onehot, axis=1) * onehot, axis=2)) - 1
    slot_index = (jnp.arange(sources, dtype=jnp.int32)[:, None] * CAP + slot_rank).astype(jnp.int32)
    token_index = (jnp.arange(STRING_LENGTH * TOP, dtype=jnp.int32) // TOP).reshape(sources, -1)
    table = jnp.zeros((EXPERTS, sources * CAP), jnp.int32).at[flat_routes, slot_index].set(token_index)
    slot_weight = jnp.zeros((EXPERTS, sources * CAP), expert_weights.dtype).at[flat_routes, slot_index].set(expert_weights.reshape(sources, -1))
    half_ff = FF // N_TP

    def expert_step(total, inputs):
        gate_matrix, up_matrix, down_matrix, index_rows, weight_rows = inputs
        batch = normed_rows[index_rows].astype(jnp.float32)
        gate_value = jnp.dot(batch, gate_matrix.astype(jnp.float32), precision=lax.Precision.HIGHEST)
        up_value = jnp.dot(batch, up_matrix.astype(jnp.float32), precision=lax.Precision.HIGHEST)
        hidden = round_trip(jax.nn.silu(gate_value) * up_value)
        summed = jnp.zeros((batch.shape[0], D), jnp.float32)
        for section in range(N_TP):
            partial_value = jnp.dot(hidden[:, section * half_ff:(section + 1) * half_ff], down_matrix[section * half_ff:(section + 1) * half_ff].astype(jnp.float32), precision=lax.Precision.HIGHEST)
            summed = summed + round_trip(partial_value)
        expert_out = round_trip(summed)
        return (total.at[index_rows].add(weight_rows[:, None] * expert_out), None)
    expert_sum, _ = lax.scan(expert_step, jnp.zeros((STRING_LENGTH, D), jnp.float32), (gate_experts, up_experts, down_experts, table, slot_weight))
    return (mixed_rows.astype(jnp.float32) + expert_sum).astype(jnp.bfloat16)
```

```python
import jax
import jax.numpy as jnp
from jax import lax
from jax.sharding import PartitionSpec as P


def swap(value):
    return lax.ppermute(value, "tp", [(0, 1), (1, 0)])


def incoming_state(total, state):
    heads, size, _ = state.shape
    count = lax.axis_size("sp")
    state = jnp.swapaxes(state, 0, 1).reshape(size, heads * size)
    total = jnp.repeat(total, size)[None, :]

    def shift(total, state, distance):
        high = total.astype(jnp.bfloat16)
        low = (total - high.astype(jnp.float32)).astype(jnp.bfloat16)
        packed = jnp.concatenate([state.astype(jnp.bfloat16), high, low], axis=0)
        got = lax.ppermute(packed, "sp", [(i, i + distance) for i in range(count - distance)])
        got = got.astype(jnp.float32)
        return got[size : size + 1] + got[size + 1 : size + 2], got[:size]

    total, state = shift(total, state, 1)
    distance = 1
    while distance < count:
        earlier_total, earlier_state = shift(total, state, distance)
        state = jnp.exp(total) * earlier_state + state
        total = total + earlier_total
        distance *= 2
    return jnp.swapaxes(state.reshape(size, heads, size), 0, 1)


def rotate(block, places):
    half_size = block.shape[-1] // 2
    frequency = 10000.0 ** (-jnp.arange(half_size, dtype=jnp.float32) / half_size)
    angles = places.astype(jnp.float32)[:, None, None] * frequency
    first_half = block[..., :half_size]
    second = block[..., half_size:]
    return jnp.concatenate(
        [
            first_half * jnp.cos(angles) - second * jnp.sin(angles),
            second * jnp.cos(angles) + first_half * jnp.sin(angles),
        ],
        axis=-1,
    )


def expert_hidden(batch, gate_matrix, up_matrix):
    gate_value = jnp.dot(batch, gate_matrix, preferred_element_type=jnp.float32)
    up_value = jnp.dot(batch, up_matrix, preferred_element_type=jnp.float32)
    return (jax.nn.silu(gate_value) * up_value).astype(jnp.bfloat16)


def shards(
    queries,
    key_vectors,
    value_vectors,
    gate_inputs,
    log_decay,
    head_gain,
    out_weight,
    residual,
    norm_gain,
    expert_ids,
    expert_weights,
    gate_experts,
    up_experts,
    down_experts,
):
    tok_dev, channels = queries.shape
    head_count = log_decay.shape[1]
    head_size = channels // head_count
    places = lax.axis_index("sp") * tok_dev + jnp.arange(tok_dev, dtype=jnp.int32)
    core = lax.axis_index("tp")
    turned_queries = rotate(
        queries.astype(jnp.float32).reshape(tok_dev, head_count, head_size), places
    )
    turned_keys = rotate(
        key_vectors.astype(jnp.float32).reshape(tok_dev, head_count, head_size), places
    ) * head_size ** (-0.5)
    value_float = value_vectors.astype(jnp.float32).reshape(tok_dev, head_count, head_size)
    running = jnp.cumsum(log_decay, axis=0)
    device_total = running[-1]
    end_weight = jnp.exp(device_total[None, :] - running)
    local_end = jnp.einsum(
        "thd,the->hde",
        turned_keys * end_weight[:, :, None],
        value_float,
        precision=lax.Precision.HIGH,
    )
    incoming = incoming_state(device_total, local_end)
    by_head = running.T
    log_gaps = by_head[:, :, None] - by_head[:, None, :]
    offsets = jnp.arange(tok_dev)
    causal = offsets[:, None] >= offsets[None, :]
    decay_weight = jnp.where(causal, jnp.exp(jnp.where(causal, log_gaps, 0.0)), 0.0)
    scores = (
        jnp.einsum("thd,shd->hts", turned_queries, turned_keys, precision=lax.Precision.HIGH)
        * decay_weight
    )
    within = jnp.einsum("hts,she->the", scores, value_float, precision=lax.Precision.HIGH)
    carried = jnp.einsum(
        "thd,hde->the",
        turned_queries * jnp.exp(running)[:, :, None],
        incoming,
        precision=lax.Precision.HIGH,
    )
    retained = within + carried
    squares = jnp.mean(retained * retained, axis=-1, keepdims=True)
    normed = retained * lax.rsqrt(squares + 1e-06) * head_gain.reshape(head_count, head_size)
    normed = (
        normed.reshape(tok_dev, channels) * jax.nn.silu(gate_inputs.astype(jnp.float32))
    ).astype(jnp.bfloat16)
    half = tok_dev // 2
    normed_away = lax.dynamic_slice_in_dim(normed, (1 - core) * half, half, 0)
    normed_here = lax.dynamic_slice_in_dim(normed, core * half, half, 0)
    away = jnp.dot(normed_away, out_weight, preferred_element_type=jnp.float32)
    got = swap(away.astype(jnp.bfloat16))
    here = jnp.dot(normed_here, out_weight, preferred_element_type=jnp.float32)
    projected = here.astype(jnp.bfloat16).astype(jnp.float32) + got.astype(jnp.float32)
    mixed_rows = (residual.astype(jnp.float32) + projected).astype(jnp.bfloat16)
    mixed_float = mixed_rows.astype(jnp.float32)
    normed_rows = (
        mixed_float
        * lax.rsqrt(jnp.mean(mixed_float * mixed_float, axis=-1, keepdims=True) + 1e-06)
        * norm_gain
    ).astype(jnp.bfloat16)
    d_model = residual.shape[1]
    experts = lax.axis_size("sp")
    capacity = 2 * tok_dev // experts
    slots = experts * capacity
    top_count = expert_ids.shape[1]
    flat_routes = expert_ids.reshape(-1)
    onehot = (flat_routes[:, None] == jnp.arange(experts, dtype=jnp.int32)[None, :]).astype(
        jnp.int32
    )
    slot_rank = jnp.sum(jnp.cumsum(onehot, axis=0) * onehot, axis=1) - 1
    slot = (flat_routes * capacity + slot_rank).reshape(-1, top_count)
    every_slot = jnp.arange(slots, dtype=jnp.int32)
    place = jnp.zeros((slots, half), jnp.bool_)
    weigh = jnp.zeros((half, slots), jnp.float32)
    for choice in range(top_count):
        column = slot[:, choice]
        place = place | (every_slot[:, None] == column[None, :])
        weigh = weigh + jnp.where(
            column[:, None] == every_slot[None, :], expert_weights[:, choice][:, None], 0.0
        )
    outgoing = jnp.dot(
        place.astype(jnp.bfloat16), normed_rows, preferred_element_type=jnp.float32
    ).astype(jnp.bfloat16)
    arrived = lax.all_to_all(
        outgoing.reshape(experts, capacity, d_model), "sp", split_axis=0, concat_axis=0, tiled=True
    ).reshape(slots, d_model)
    partner = swap(arrived)
    hidden_here = expert_hidden(arrived, gate_experts[0], up_experts[0])
    hidden_away = expert_hidden(partner, gate_experts[0], up_experts[0])
    part_away = jnp.dot(hidden_away, down_experts[0], preferred_element_type=jnp.float32)
    got_part = swap(part_away.astype(jnp.bfloat16))
    part_here = jnp.dot(hidden_here, down_experts[0], preferred_element_type=jnp.float32)
    summed = (
        part_here.astype(jnp.bfloat16).astype(jnp.float32) + got_part.astype(jnp.float32)
    ).astype(jnp.bfloat16)
    returned = lax.all_to_all(
        summed.reshape(experts, capacity, d_model), "sp", split_axis=0, concat_axis=0, tiled=True
    ).reshape(slots, d_model)
    weigh_high = weigh.astype(jnp.bfloat16)
    weigh_low = (weigh - weigh_high.astype(jnp.float32)).astype(jnp.bfloat16)
    expert_sum = jnp.dot(weigh_high, returned, preferred_element_type=jnp.float32) + jnp.dot(
        weigh_low, returned, preferred_element_type=jnp.float32
    )
    return (mixed_float + expert_sum).astype(jnp.bfloat16)


def solution(mesh):
    return jax.shard_map(
        shards,
        mesh=mesh,
        in_specs=(
            P("sp", "tp"),
            P("sp", "tp"),
            P("sp", "tp"),
            P("sp", "tp"),
            P("sp", "tp"),
            P("tp"),
            P("tp", None),
            P(("sp", "tp"), None),
            P(),
            P(("sp", "tp"), None),
            P(("sp", "tp"), None),
            P("sp", None, "tp"),
            P("sp", None, "tp"),
            P("sp", "tp", None),
        ),
        out_specs=P(("sp", "tp"), None),
        check_vma=False,
    )
```

```python
import jax
import jax.numpy as jnp
from jax import lax
from jax.sharding import PartitionSpec as P


def swap(value):
    return lax.ppermute(value, "tp", [(0, 1), (1, 0)])


def incoming_state(total, state):
    heads, size, _ = state.shape
    count = lax.axis_size("sp")
    state = jnp.swapaxes(state, 0, 1).reshape(size, heads * size)
    total = jnp.repeat(total, size)[None, :]

    def shift(total, state, distance):
        high = total.astype(jnp.bfloat16)
        low = (total - high.astype(jnp.float32)).astype(jnp.bfloat16)
        packed = jnp.concatenate([state.astype(jnp.bfloat16), high, low], axis=0)
        got = lax.ppermute(packed, "sp", [(i, i + distance) for i in range(count - distance)])
        got = got.astype(jnp.float32)
        return got[size : size + 1] + got[size + 1 : size + 2], got[:size]

    before_total, before_state = jnp.zeros_like(total), jnp.zeros_like(state)
    distance = 1
    while distance < count:
        earlier_total, earlier_state = shift(total, state, distance)
        before_state = jnp.exp(before_total) * earlier_state + before_state
        before_total = before_total + earlier_total
        state = jnp.exp(total) * earlier_state + state
        total = total + earlier_total
        distance *= 2
    return jnp.swapaxes(before_state.reshape(size, heads, size), 0, 1)


def rotate(block, places):
    half_size = block.shape[-1] // 2
    frequency = 10000.0 ** (-jnp.arange(half_size, dtype=jnp.float32) / half_size)
    angles = places.astype(jnp.float32)[:, None, None] * frequency
    first_half = block[..., :half_size]
    second = block[..., half_size:]
    return jnp.concatenate(
        [
            first_half * jnp.cos(angles) - second * jnp.sin(angles),
            second * jnp.cos(angles) + first_half * jnp.sin(angles),
        ],
        axis=-1,
    )


def expert_hidden(batch, gate_matrix, up_matrix):
    gate_value = jnp.dot(batch, gate_matrix, preferred_element_type=jnp.float32)
    up_value = jnp.dot(batch, up_matrix, preferred_element_type=jnp.float32)
    return (jax.nn.silu(gate_value) * up_value).astype(jnp.bfloat16)


def shards(
    queries,
    key_vectors,
    value_vectors,
    gate_inputs,
    log_decay,
    head_gain,
    out_weight,
    residual,
    norm_gain,
    expert_ids,
    expert_weights,
    gate_experts,
    up_experts,
    down_experts,
):
    tok_dev, channels = queries.shape
    head_count = log_decay.shape[1]
    head_size = channels // head_count
    places = lax.axis_index("sp") * tok_dev + jnp.arange(tok_dev, dtype=jnp.int32)
    core = lax.axis_index("tp")
    turned_queries = rotate(
        queries.astype(jnp.float32).reshape(tok_dev, head_count, head_size), places
    )
    turned_keys = rotate(
        key_vectors.astype(jnp.float32).reshape(tok_dev, head_count, head_size), places
    ) * head_size ** (-0.5)
    value_float = value_vectors.astype(jnp.float32).reshape(tok_dev, head_count, head_size)
    running = jnp.cumsum(log_decay, axis=0)
    device_total = running[-1]
    end_weight = jnp.exp(device_total[None, :] - running)
    local_end = jnp.einsum(
        "thd,the->hde",
        turned_keys * end_weight[:, :, None],
        value_float,
        precision=lax.Precision.HIGH,
    )
    incoming = incoming_state(device_total, local_end)
    by_head = running.T
    log_gaps = by_head[:, :, None] - by_head[:, None, :]
    offsets = jnp.arange(tok_dev)
    causal = offsets[:, None] >= offsets[None, :]
    decay_weight = jnp.where(causal, jnp.exp(jnp.where(causal, log_gaps, 0.0)), 0.0)
    scores = (
        jnp.einsum("thd,shd->hts", turned_queries, turned_keys, precision=lax.Precision.HIGH)
        * decay_weight
    )
    within = jnp.einsum("hts,she->the", scores, value_float, precision=lax.Precision.HIGH)
    carried = jnp.einsum(
        "thd,hde->the",
        turned_queries * jnp.exp(running)[:, :, None],
        incoming,
        precision=lax.Precision.HIGH,
    )
    retained = within + carried
    squares = jnp.mean(retained * retained, axis=-1, keepdims=True)
    normed = retained * lax.rsqrt(squares + 1e-06) * head_gain.reshape(head_count, head_size)
    normed = (
        normed.reshape(tok_dev, channels) * jax.nn.silu(gate_inputs.astype(jnp.float32))
    ).astype(jnp.bfloat16)
    half = tok_dev // 2
    normed_away = lax.dynamic_slice_in_dim(normed, (1 - core) * half, half, 0)
    normed_here = lax.dynamic_slice_in_dim(normed, core * half, half, 0)
    away = jnp.dot(normed_away, out_weight, preferred_element_type=jnp.float32)
    got = swap(away.astype(jnp.bfloat16))
    here = jnp.dot(normed_here, out_weight, preferred_element_type=jnp.float32)
    projected = here.astype(jnp.bfloat16).astype(jnp.float32) + got.astype(jnp.float32)
    mixed_rows = (residual.astype(jnp.float32) + projected).astype(jnp.bfloat16)
    mixed_float = mixed_rows.astype(jnp.float32)
    normed_rows = (
        mixed_float
        * lax.rsqrt(jnp.mean(mixed_float * mixed_float, axis=-1, keepdims=True) + 1e-06)
        * norm_gain
    ).astype(jnp.bfloat16)
    d_model = residual.shape[1]
    experts = lax.axis_size("sp")
    capacity = 2 * tok_dev // experts
    slots = experts * capacity
    top_count = expert_ids.shape[1]
    flat_routes = expert_ids.reshape(-1)
    onehot = (flat_routes[:, None] == jnp.arange(experts, dtype=jnp.int32)[None, :]).astype(
        jnp.int32
    )
    slot_rank = jnp.sum(jnp.cumsum(onehot, axis=0) * onehot, axis=1) - 1
    slot = (flat_routes * capacity + slot_rank).reshape(-1, top_count)
    every_slot = jnp.arange(slots, dtype=jnp.int32)
    place = jnp.zeros((slots, half), jnp.bool_)
    weigh = jnp.zeros((half, slots), jnp.float32)
    for choice in range(top_count):
        column = slot[:, choice]
        place = place | (every_slot[:, None] == column[None, :])
        weigh = weigh + jnp.where(
            column[:, None] == every_slot[None, :], expert_weights[:, choice][:, None], 0.0
        )
    outgoing = jnp.dot(
        place.astype(jnp.bfloat16), normed_rows, preferred_element_type=jnp.float32
    ).astype(jnp.bfloat16)
    arrived = lax.all_to_all(
        outgoing.reshape(experts, capacity, d_model), "sp", split_axis=0, concat_axis=0, tiled=True
    ).reshape(slots, d_model)
    both = jnp.concatenate([swap(arrived), arrived], axis=0)
    hidden = expert_hidden(both, gate_experts[0], up_experts[0])
    part = jnp.dot(hidden, down_experts[0], preferred_element_type=jnp.float32).astype(
        jnp.bfloat16
    )
    got_part = swap(part[:slots])
    part_here = part[slots:]
    summed = (
        part_here.astype(jnp.float32) + got_part.astype(jnp.float32)
    ).astype(jnp.bfloat16)
    returned = lax.all_to_all(
        summed.reshape(experts, capacity, d_model), "sp", split_axis=0, concat_axis=0, tiled=True
    ).reshape(slots, d_model)
    weigh_high = weigh.astype(jnp.bfloat16)
    weigh_low = (weigh - weigh_high.astype(jnp.float32)).astype(jnp.bfloat16)
    expert_sum = jnp.dot(weigh_high, returned, preferred_element_type=jnp.float32) + jnp.dot(
        weigh_low, returned, preferred_element_type=jnp.float32
    )
    return (mixed_float + expert_sum).astype(jnp.bfloat16)


def solution(mesh):
    return jax.shard_map(
        shards,
        mesh=mesh,
        in_specs=(
            P("sp", "tp"),
            P("sp", "tp"),
            P("sp", "tp"),
            P("sp", "tp"),
            P("sp", "tp"),
            P("tp"),
            P("tp", None),
            P(("sp", "tp"), None),
            P(),
            P(("sp", "tp"), None),
            P(("sp", "tp"), None),
            P("sp", None, "tp"),
            P("sp", None, "tp"),
            P("sp", "tp", None),
        ),
        out_specs=P(("sp", "tp"), None),
        check_vma=False,
    )
```
